128 devices in a mesh: sp: 32 (over z, y, core), tp: 4 (over x).
Axes of the slice: x: 4, y: 4, z: 4, core: 2. Of those that a mesh axis runs over, the one named last changes fastest.
Arguments:
- tokens: bfloat16 [12288, 2048], P(('sp', 'tp')), may hold values from -8 to 8, as said below
- query_weight: bfloat16 [2048, 1024], P(None, 'tp'), as said below
- key_weight: bfloat16 [2048, 256], P(None, 'tp'), as said below
- value_weight: bfloat16 [2048, 256], P(None, 'tp'), may hold values from -0.125 to 0.125
- out_weight: bfloat16 [1024, 2048], P('tp'), may hold values from -0.75 to 0.75
- query_gain: bfloat16 [16, 64], P('tp'), may hold values from 0.5 to 6.5
- key_gain: bfloat16 [4, 64], P('tp'), may hold values from 0.5 to 6.5
Outputs:
- mixed: bfloat16 [12288, 2048], P(('sp', 'tp'))
- log_sums: float32 [16, 12288], P('tp', 'sp')
The draws below stay inside these ranges and needn't reach their ends.
Inputs may be any that keep to these rules, and one draw needn't show every extreme that they name: Each block of 384 consecutive tokens has a mean vector of its own. `query_weight`: entries are those of a weight over 2048 inputs, of magnitude at most 6 / sqrt(2048). `key_weight`: entries are those of a weight over 2048 inputs, of magnitude at most 6 / sqrt(2048).
All inputs are finite; a program needn't handle non-finite values.
Results may differ from the reference program's by a relative error of at most 0.028.
Values may be sent and summed in bfloat16 or wider, within the bound.
No kernel may reach another device: no remote copies, remote signals or barrier semaphores. Data moves between devices by JAX's collectives and lax.ppermute only.
A program may use at most 64 MiB of HBM per device.

```python
import math
import jax
import jax.numpy as jnp
from jax import lax

D = 2048
HEADS = 16
KV_HEADS = 4
HD = 64
GRID_W = 64
TOK_DEV = 384
TOKENS = 12288
N_TP = 4


def shared_query(key):
    base = jnp.clip(jax.random.normal(jax.random.fold_in(key, 11), (D, HEADS * HD), jnp.float32), -6.0, 6.0)
    base = base * D ** (-0.5)
    return base


def draw_tokens(key, part):
    offsets = jax.random.normal(jax.random.fold_in(key, 21), (TOKENS // TOK_DEV, D), jnp.float32)
    offsets = jnp.repeat(offsets, TOK_DEV, axis=0)
    noise = jax.random.normal(jax.random.fold_in(key, 22), (TOKENS, D), jnp.float32)
    return jnp.clip(noise + offsets, -8.0, 8.0).astype(jnp.bfloat16)


def draw_query_weight(key, part):
    return shared_query(key).astype(jnp.bfloat16)


def draw_key_weight(key, part):
    base = jnp.clip(jax.random.normal(jax.random.fold_in(key, 12), (D, KV_HEADS * HD), jnp.float32), -6.0, 6.0)
    return (base * D ** (-0.5)).astype(jnp.bfloat16)


def draw_query_gain(key, part):
    usual = jax.random.uniform(jax.random.fold_in(key, 31), (HEADS, HD), jnp.float32, 0.5, 1.5)
    return usual.astype(jnp.bfloat16)


def draw_key_gain(key, part):
    return jax.random.uniform(jax.random.fold_in(key, 41), (KV_HEADS, HD), jnp.float32, 0.5, 1.5).astype(jnp.bfloat16)


def level_of(key, shape, shards, low, largest):
    loudness = 1.0
    for dim, blocks in shards:
        draws = jax.random.uniform(jax.random.fold_in(jax.random.fold_in(key, 6), dim), (blocks,), jnp.float32, low / len(shards), largest / len(shards))
        loudness = loudness * jnp.repeat(jnp.exp(draws), shape[dim] // blocks).reshape((-1,) + (1,) * (len(shape) - 1 - dim))
    return loudness


def bell_draw(stream_key, dims, scale, reach, shards=(), held_as=jnp.bfloat16):
    loudness = level_of(stream_key, dims, shards, -0.22, 0.18) if shards else 1.0
    drawn = jax.random.normal(stream_key, dims, jnp.float32) * scale * loudness
    return jnp.minimum(jnp.maximum(drawn, -reach), reach).astype(held_as)


def setup_inputs(seed: int = 0) -> dict:
    key_of = jax.random.split(jax.random.key(seed), 8)
    return {
        "tokens": draw_tokens(jax.random.fold_in(key_of[7], 71), 0),
        "query_weight": draw_query_weight(jax.random.fold_in(key_of[7], 71), 0),
        "key_weight": draw_key_weight(jax.random.fold_in(key_of[7], 71), 0),
        "value_weight": bell_draw(key_of[3], (D, KV_HEADS * HD), D ** -0.5, 0.125, ((1, 4),)),
        "out_weight": bell_draw(key_of[4], (HEADS * HD, D), (HEADS * HD // 16) ** -0.5, 0.75, ((0, 4),)),
        "query_gain": draw_query_gain(jax.random.fold_in(key_of[7], 71), 0),
        "key_gain": draw_key_gain(jax.random.fold_in(key_of[7], 71), 0),
    }


def angle_tables(count):
    quarter = HD // 4
    place = jnp.arange(count, dtype=jnp.int32)
    grid_row = (place // GRID_W).astype(jnp.float32)
    grid_col = (place % GRID_W).astype(jnp.float32)
    freq = 10000.0 ** (-jnp.arange(quarter, dtype=jnp.float32).astype(jnp.float32) / quarter)
    row_angle = grid_row[:, None] * freq[None, :]
    col_angle = grid_col[:, None] * freq[None, :]
    return (jnp.cos(row_angle), jnp.sin(row_angle), jnp.cos(col_angle), jnp.sin(col_angle))

def turn_pairs(part, cosine, sine):
    quarter = part.shape[-1] // 2
    first = part[..., :quarter]
    second = part[..., quarter:]
    cosine = cosine[:, None, :]
    sine = sine[:, None, :]
    return jnp.concatenate([first * cosine - second * sine, second * cosine + first * sine], axis=-1)

def prepare(raw, gain, tables):
    count = raw.shape[0]
    heads = gain.shape[0]
    values = raw.astype(jnp.float32).reshape(count, heads, HD)
    scaled = values * lax.rsqrt(lax.optimization_barrier(jnp.mean(values * values, axis=-1, keepdims=True)) + 1e-06)
    scaled = scaled * gain.astype(jnp.float32)[None, :, :]
    half = HD // 2
    row_cos, row_sin, col_cos, col_sin = tables
    turned = jnp.concatenate([turn_pairs(scaled[..., :half], row_cos, row_sin), turn_pairs(scaled[..., half:], col_cos, col_sin)], axis=-1)
    return turned.astype(jnp.bfloat16)

def reference(tokens, query_weight, key_weight, value_weight, out_weight, query_gain, key_gain):
    count = tokens.shape[0]
    query_raw = jnp.dot(tokens, query_weight, preferred_element_type=jnp.float32).astype(jnp.bfloat16)
    key_raw = jnp.dot(tokens, key_weight, preferred_element_type=jnp.float32).astype(jnp.bfloat16)
    values = jnp.dot(tokens, value_weight, preferred_element_type=jnp.float32).astype(jnp.bfloat16)
    tables = angle_tables(count)
    queries = prepare(query_raw, query_gain, tables)
    keys = prepare(key_raw, key_gain, tables)
    share = HEADS // KV_HEADS
    key_float = keys.astype(jnp.float32)
    value_float = values.reshape(count, KV_HEADS, HD).astype(jnp.float32)
    block_len = math.gcd(count, 128)
    blocks = queries.reshape(count // block_len, block_len, KV_HEADS, share, HD)

    def one_block(query_block):
        scores = jnp.einsum('qhgd,khd->hgqk', query_block.astype(jnp.float32), key_float, precision=lax.Precision.HIGHEST) * HD ** (-0.5)
        row_max = lax.optimization_barrier(jnp.max(scores, axis=-1))
        expo = jnp.exp(scores - row_max[..., None])
        totals = lax.optimization_barrier(jnp.sum(expo, axis=-1))
        weights = lax.optimization_barrier(expo.astype(jnp.bfloat16)).astype(jnp.float32)
        summed = jnp.einsum('hgqk,khd->qhgd', weights, value_float, precision=lax.Precision.HIGHEST)
        attended = summed / jnp.transpose(totals, (2, 0, 1))[..., None]
        log_block = (row_max + jnp.log(totals)).reshape(HEADS, block_len)
        return (attended.astype(jnp.bfloat16).reshape(block_len, HEADS * HD), log_block)
    attended, log_blocks = lax.map(one_block, blocks)
    attended = attended.reshape(count, HEADS * HD)
    log_sums = jnp.transpose(log_blocks, (1, 0, 2)).reshape(HEADS, count)
    group_width = HEADS // N_TP * HD
    total = jnp.zeros((count, D), jnp.float32)
    for group in range(N_TP):
        lo = group * group_width
        partial_sum = jnp.dot(attended[:, lo:lo + group_width], out_weight[lo:lo + group_width], preferred_element_type=jnp.float32).astype(jnp.bfloat16)
        total = total + partial_sum.astype(jnp.float32)
    return (total.astype(jnp.bfloat16), log_sums)
```

```python
import functools

import jax
import jax.numpy as jnp
from jax import lax
from jax.experimental import pallas as pl
from jax.experimental.pallas import tpu as pltpu
from jax.sharding import PartitionSpec as P

GRID_W = 64
ROPE_BASE = 10000.0
LOG2E = 1.4426950408889634
HEADROOM = 40.0
SUM_LOW = 2.0**-80
SUM_HIGH = 2.0**100
VMEM = pl.BlockSpec(memory_space=pltpu.VMEM)
QT = 768
KT = 768


def ring(n, k):
    return [(i, (i + k) % n) for i in range(n)]


def grid_move(step, first):
    pairs = []
    for s in range(32):
        z, y, c = s // 8, (s // 2) % 4, s % 2
        if (c == 0) == first:
            z = (z + step) % 4
        else:
            y = (y + step) % 4
        pairs.append((s, z * 8 + y * 2 + c))
    return pairs


def core_swap():
    return [(s, s ^ 1) for s in range(32)]


def dot(a, b):
    return lax.dot_general(a, b, (((1,), (0,)), ((), ())), preferred_element_type=jnp.float32)


def angle_rows(first_blocks, count, quarter):
    place = jnp.concatenate([f + jnp.arange(count, dtype=jnp.int32) for f in first_blocks])
    grid_row = (place // GRID_W).astype(jnp.float32)
    grid_col = (place % GRID_W).astype(jnp.float32)
    freq = ROPE_BASE ** (-jnp.arange(quarter, dtype=jnp.float32) / quarter)
    row_angle = freq[:, None] * grid_row[None, :]
    col_angle = freq[:, None] * grid_col[None, :]
    return jnp.concatenate(
        [jnp.cos(row_angle), jnp.sin(row_angle), jnp.cos(col_angle), jnp.sin(col_angle)], axis=0
    )


def project_kernel(t0, t1, t2, t3, wq, wkv, gq, gk, tab, qt_ref, kv_ref, raw):
    n = t0.shape[0]
    for i, t in enumerate((t0, t1, t2, t3)):
        x = t[...]
        raw[i * n : (i + 1) * n, :256] = dot(x, wq[...]).astype(jnp.bfloat16)
        raw[i * n : (i + 1) * n, 256:] = dot(x, wkv[...]).astype(jnp.bfloat16)
    table = tab[...]
    rc, rs, cc, cs = table[0:16], table[16:32], table[32:48], table[48:64]

    def norm_turn(x, gain):
        x = x * lax.rsqrt(jnp.mean(x * x, axis=0, keepdims=True) + 1e-06)
        x = x * gain
        a, b, c, d = x[0:16], x[16:32], x[32:48], x[48:64]
        return jnp.concatenate(
            [a * rc - b * rs, b * rc + a * rs, c * cc - d * cs, d * cc + c * cs], axis=0
        )

    count = raw.shape[0]
    for h in range(4):
        if h % 2 == 0:
            both = raw[:, h * 64 : h * 64 + 128].astype(jnp.float32).T
        x = both[(h % 2) * 64 : (h % 2) * 64 + 64]
        q = norm_turn(x, gq[:, h : h + 1]).astype(jnp.bfloat16)
        qt_ref[0:64, h * count : (h + 1) * count] = q
        qt_ref[64:128, h * count : (h + 1) * count] = jnp.zeros_like(q)
    kv = raw[:, 256:384].astype(jnp.float32).T
    keys = norm_turn(kv[0:64], gk[...])
    kv_ref[...] = jnp.concatenate([keys, kv[64:128]], axis=0).T.astype(jnp.bfloat16)


def attend_kernel(*refs, n_kv, n_extra, first, last, scale):
    refs = list(refs)
    qt_ref = refs.pop(0)
    kv_refs = [refs.pop(0) for _ in range(n_kv)]
    extra = [refs.pop(0) for _ in range(n_extra)]
    if not first:
        acc_in, l_in, m_in = [refs.pop(0) for _ in range(3)]
    if last:
        att_ref, lse_ref = [refs.pop(0) for _ in range(2)]
        acc_ref, l_ref, m_ref = [refs.pop(0) for _ in range(3)]
    else:
        acc_ref, l_ref, m_ref = [refs.pop(0) for _ in range(3)]
    vt_ref, p_ref = refs
    c = scale * LOG2E
    nq = qt_ref.shape[1]
    rows = kv_refs[0].shape[0]
    per = rows // KT

    for j, kv in enumerate(kv_refs):

        def flip(i, _):
            r = pl.multiple_of(i * KT, KT)
            vt_ref[j * per + i] = kv[pl.ds(r, KT), :].T[64:, :]
            return 0

        lax.fori_loop(0, per, flip, 0, unroll=True)

    for qi in range(nq // QT):
        cols = slice(qi * QT, (qi + 1) * QT)
        if first:
            top = None
            for kv in kv_refs:
                for b in range(rows // 384):
                    s = dot(kv[b * 384 : b * 384 + 64, :], qt_ref[:, cols])
                    s = jnp.max(s, axis=0, keepdims=True)
                    top = s if top is None else jnp.maximum(top, s)
            m_ref[:, cols] = top * c + HEADROOM
            acc_ref[:, cols] = jnp.zeros((64, QT), jnp.float32)
            l_ref[:, cols] = jnp.zeros((8, QT), jnp.float32)
        else:
            m_ref[:, cols] = m_in[:, cols]
            acc_ref[:, cols] = acc_in[:, cols]
            l_ref[:, cols] = l_in[:, cols]

    def weigh(kv, i, slot, cols):
        s = dot(kv[i * KT : (i + 1) * KT, :], qt_ref[:, cols])
        p = jnp.exp2(s * c - m_ref[:, cols])
        l_ref[:, cols] += jnp.sum(p.reshape(KT // 8, 8, QT), axis=0)
        p_ref[slot] = p.astype(jnp.bfloat16)

    def gather_values(j, slot, cols):
        acc_ref[:, cols] += dot(vt_ref[j], p_ref[slot])

    steps = [
        (kv, i, j * per + i, slice(qi * QT, (qi + 1) * QT))
        for qi in range(nq // QT)
        for j, kv in enumerate(kv_refs)
        for i in range(per)
    ]
    before = None
    for t, (kv, i, j, cols) in enumerate(steps):
        weigh(kv, i, t % 2, cols)
        if before is not None:
            gather_values(*before)
        before = (j, t % 2, cols)
    gather_values(*before)

    if last:
        total = jnp.sum(l_ref[...], axis=0, keepdims=True)
        good = jnp.logical_and(total > SUM_LOW, total < SUM_HIGH)
        n_bad = jnp.sum(jnp.where(good, 0.0, 1.0))

        @pl.when(n_bad > 0.0)
        def _():
            every = list(extra) + list(kv_refs)
            for qi in range(nq // 128):
                cols = slice(qi * 128, (qi + 1) * 128)
                m_ref[:, cols] = jnp.full((1, 128), -3e38, jnp.float32)
                acc_ref[:, cols] = jnp.zeros((64, 128), jnp.float32)
                l_ref[:, cols] = jnp.zeros((8, 128), jnp.float32)
            for kv in every:

                def top_of(i, _):
                    r = pl.multiple_of(i * 128, 128)
                    s = dot(kv[pl.ds(r, 128), :], qt_ref[...])
                    m_ref[...] = jnp.maximum(m_ref[...], jnp.max(s, axis=0, keepdims=True) * c)
                    return 0

                lax.fori_loop(0, rows // 128, top_of, 0)
            for kv in every:

                def again(i, _):
                    r = pl.multiple_of(i * 128, 128)
                    blk = kv[pl.ds(r, 128), :]
                    p = jnp.exp2(dot(blk, qt_ref[...]) * c - m_ref[...])
                    l_ref[...] += jnp.sum(p.reshape(16, 8, nq), axis=0)
                    acc_ref[...] += dot(blk.T[64:, :], p.astype(jnp.bfloat16))
                    return 0

                lax.fori_loop(0, rows // 128, again, 0)

        total = jnp.sum(l_ref[...], axis=0, keepdims=True)
        lse = (m_ref[...] + jnp.log2(total)) * (1.0 / LOG2E)
        out = acc_ref[...] / total
        count = nq // 4
        for h in range(0, 4, 2):
            two = jnp.concatenate(
                [out[:, h * count : (h + 1) * count], out[:, (h + 1) * count : (h + 2) * count]], axis=0
            )
            att_ref[:, h * 64 : h * 64 + 128] = two.T.astype(jnp.bfloat16)
        for h in range(4):
            lse_ref[h : h + 1, :] = lse[:, h * count : (h + 1) * count]


def attend(qt, kvs, extra, state, last, scale):
    nq = qt.shape[1]
    rows = kvs[0].shape[0]
    keys = rows * len(kvs)
    f32 = jnp.float32
    parts = (jax.ShapeDtypeStruct((64, nq), f32), jax.ShapeDtypeStruct((8, nq), f32), jax.ShapeDtypeStruct((1, nq), f32))
    scratch = [pltpu.VMEM((keys // KT, 64, KT), jnp.bfloat16), pltpu.VMEM((2, KT, QT), jnp.bfloat16)]
    if last:
        outs = (jax.ShapeDtypeStruct((nq // 4, 256), jnp.bfloat16), jax.ShapeDtypeStruct((4, nq // 4), f32))
        scratch = [pltpu.VMEM(p.shape, f32) for p in parts] + scratch
    else:
        outs = parts
    args = [qt, *kvs, *extra, *(state or ())]
    return pl.pallas_call(
        functools.partial(
            attend_kernel, n_kv=len(kvs), n_extra=len(extra), first=state is None, last=last, scale=scale
        ),
        out_shape=outs,
        in_specs=[VMEM] * len(args),
        out_specs=(VMEM,) * len(outs),
        scratch_shapes=scratch,
        compiler_params=pltpu.CompilerParams(vmem_limit_bytes=40 * 2**20),
        cost_estimate=pl.CostEstimate(
            flops=4 * nq * keys * 64, bytes_accessed=keys * 256 + nq * 512, transcendentals=nq * keys
        ),
    )(*args)


def mix_kernel(core, a0, a1, a2, a3, w0, w1, w2, w3, x1, x2, x3, out_ref):
    half = w1.shape[1]
    here = pl.multiple_of(core[0] * half, half)
    there = pl.multiple_of((1 - core[0]) * half, half)
    own = a0[...]
    near = dot(own, w0[:, pl.ds(here, half)])
    far = dot(own, w0[:, pl.ds(there, half)])
    for a, w, x in ((a1, w1, x1), (a2, w2, x2), (a3, w3, x3)):
        near += dot(a[...], w[...])
        far += dot(a[...], x[...])
    out_ref[:, pl.ds(here, half)] = near.astype(jnp.bfloat16)
    out_ref[:, pl.ds(there, half)] = far.astype(jnp.bfloat16)


def body(tokens, query_weight, key_weight, value_weight, out_weight, query_gain, key_gain):
    scale = query_gain.shape[1] ** (-0.5)
    n = tokens.shape[0]
    sp, tp = lax.axis_index("sp"), lax.axis_index("tp")
    core = sp % 2
    from_left = lax.ppermute(tokens, "tp", ring(4, 1))
    from_right = lax.ppermute(tokens, "tp", ring(4, 3))
    from_far = lax.ppermute(tokens, "tp", ring(4, 2))
    wkv = jnp.concatenate([key_weight, value_weight], axis=1)
    firsts = [sp * (4 * n) + ((tp + k) % 4) * n for k in (0, 3, 1, 2)]
    table = angle_rows(firsts, n, 16)
    gq = query_gain.astype(jnp.float32).T
    gk = key_gain.astype(jnp.float32).T
    qt, kv = pl.pallas_call(
        project_kernel,
        out_shape=(
            jax.ShapeDtypeStruct((128, 16 * n), jnp.bfloat16),
            jax.ShapeDtypeStruct((4 * n, 128), jnp.bfloat16),
        ),
        in_specs=[VMEM] * 9,
        out_specs=(VMEM, VMEM),
        scratch_shapes=[pltpu.VMEM((4 * n, 384), jnp.bfloat16)],
        compiler_params=pltpu.CompilerParams(vmem_limit_bytes=30 * 2**20),
        cost_estimate=pl.CostEstimate(flops=2 * 4 * n * 2048 * 384, bytes_accessed=2**22, transcendentals=0),
    )(tokens, from_left, from_right, from_far, query_weight, wkv, gq, gk, table)

    line = [kv] + [lax.ppermute(kv, "sp", grid_move(k, True)) for k in (1, 3, 2)]
    line = jnp.concatenate(line, axis=0)
    plane = [lax.ppermute(line, "sp", grid_move(k, False)) for k in (1, 3, 2)]
    swapped = lax.ppermute(line, "sp", core_swap())
    twins = [lax.ppermute(p, "sp", core_swap()) for p in plane]

    half = out_weight.shape[1] // 2
    mine = lax.dynamic_slice_in_dim(out_weight, core * half, half, axis=1)
    rows_in = [lax.ppermute(mine, "tp", ring(4, k)) for k in (1, 3, 2)]
    rows_other = [lax.ppermute(w, "sp", core_swap()) for w in rows_in]

    state = attend(qt, [line, swapped], [], None, False, scale)
    state = attend(qt, plane, [], state, False, scale)
    att, lse = attend(qt, twins, [line, swapped, *plane], state, True, scale)

    back = [lax.ppermute(att[i * n : (i + 1) * n], "tp", ring(4, k)) for i, k in ((2, 1), (1, 3), (3, 2))]
    mixed = pl.pallas_call(
        mix_kernel,
        out_shape=jax.ShapeDtypeStruct((n, 2 * half), jnp.bfloat16),
        in_specs=[pl.BlockSpec(memory_space=pltpu.SMEM)] + [VMEM] * 11,
        out_specs=VMEM,
        compiler_params=pltpu.CompilerParams(vmem_limit_bytes=30 * 2**20),
        cost_estimate=pl.CostEstimate(flops=2 * n * 1024 * 2048, bytes_accessed=2**22, transcendentals=0),
    )(core.reshape(1), att[:n], *back, out_weight, *rows_in, *rows_other)

    cyc = [lse[:, i * n : (i + 1) * n] for i in (0, 2, 3, 1)]
    turned = [jnp.concatenate([cyc[(a - t) % 4] for a in range(4)], axis=1) for t in range(4)]
    log_sums = jnp.where(tp == 0, turned[0], jnp.where(tp == 1, turned[1], jnp.where(tp == 2, turned[2], turned[3])))
    return (mixed, log_sums)


def solution(mesh):
    return jax.shard_map(
        body,
        mesh=mesh,
        in_specs=(
            P(("sp", "tp"), None),
            P(None, "tp"),
            P(None, "tp"),
            P(None, "tp"),
            P("tp", None),
            P("tp", None),
            P("tp", None),
        ),
        out_specs=(P(("sp", "tp"), None), P("tp", "sp")),
        check_vma=False,
    )
```

```python
import functools

import jax
import jax.numpy as jnp
import numpy as np
from jax import lax
from jax.experimental import pallas as pl
from jax.experimental.pallas import tpu as pltpu
from jax.sharding import PartitionSpec as P


ROPE_BASE = 10000.0
LOG2E = 1.4426950408889634
HEADROOM = 40.0
SUM_LOW = 2.0**-80
SUM_HIGH = 2.0**100
VMEM = pl.BlockSpec(memory_space=pltpu.VMEM)
QT = 768
KT = 768


def ring(n, k):
    return [(i, (i + k) % n) for i in range(n)]


def grid_move(step, first):
    pairs = []
    for s in range(32):
        z, y, c = s // 8, (s // 2) % 4, s % 2
        if (c == 0) == first:
            z = (z + step) % 4
        else:
            y = (y + step) % 4
        pairs.append((s, z * 8 + y * 2 + c))
    return pairs


def core_swap():
    return [(s, s ^ 1) for s in range(32)]


def dot(a, b):
    return lax.dot_general(a, b, (((1,), (0,)), ((), ())), preferred_element_type=jnp.float32)


def angle_rows(sp, tp, n):
    lane = lax.broadcasted_iota(jnp.int32, (64, 512), 1)
    row = lax.broadcasted_iota(jnp.int32, (64, 512), 0)
    again = lane >= 4 * n
    block = jnp.where(again, 3, lax.div(lane, n))
    inside = jnp.where(again, lane - 4 * n, lax.rem(lane, n))
    shift = jnp.where(block == 0, 0, jnp.where(block == 1, 3, jnp.where(block == 2, 1, 2)))
    place = sp * (4 * n) + ((tp + shift) & 3) * n + inside
    freq = jnp.asarray(np.tile(ROPE_BASE ** (-np.arange(16) / 16.0), 4)[:, None], jnp.float32)
    angle = jnp.where(row < 32, place >> 6, place & 63).astype(jnp.float32) * freq
    return jnp.where((row & 16) == 0, jnp.cos(angle), jnp.sin(angle))


def column(gain):
    eye = lax.broadcasted_iota(jnp.int32, (64, 64), 0) == lax.broadcasted_iota(jnp.int32, (64, 64), 1)
    wide = jnp.broadcast_to(gain.astype(jnp.float32), (64, 64))
    return jnp.sum(jnp.where(eye, wide, 0.0), axis=1, keepdims=True)


def norm_turn(x, gain, table):
    x = x * lax.rsqrt(jnp.mean(x * x, axis=0, keepdims=True) + 1e-06)
    x = x * gain
    rc, rs, cc, cs = table[0:16], table[16:32], table[32:48], table[48:64]
    a, b, c, d = x[0:16], x[16:32], x[32:48], x[48:64]
    return jnp.concatenate(
        [a * rc - b * rs, b * rc + a * rs, c * cc - d * cs, d * cc + c * cs], axis=0
    )


def keys_values(raw, gain, table):
    kv = raw.astype(jnp.float32).T
    keys = norm_turn(kv[0:64], gain, table)
    return jnp.concatenate([keys, kv[64:128]], axis=0).T.astype(jnp.bfloat16)


def own_kernel(place, t0, wq, wk, wv, wo, raw_ref, weight_ref, wo_ref):
    weight_ref[:, :256] = wq[...]
    weight_ref[:, 256:] = jnp.concatenate([wk[...], wv[...]], axis=0).astype(jnp.float32).T.astype(jnp.bfloat16)
    raw_ref[...] = dot(t0[...], weight_ref[...]).astype(jnp.bfloat16)
    half = wo_ref.shape[0]
    wo_ref[...] = wo[pl.ds(pl.multiple_of(place[0] * half, half), half), :]


def near_kernel(raw_own, t1, t2, weight, gk, tab, raw_ref, kv_ref, raw):
    n = t1.shape[0]
    raw[3 * n :, :] = jnp.zeros((n, 128), jnp.bfloat16)
    raw[:n, :] = raw_own[:, 256:]
    raw_ref[:n, :] = raw_own[:, :256]
    for i, t in ((1, t1), (2, t2)):
        made = dot(t[...], weight[...]).astype(jnp.bfloat16)
        raw[i * n : (i + 1) * n, :] = made[:, 256:]
        raw_ref[i * n : (i + 1) * n, :] = made[:, :256]
    kv_ref[...] = keys_values(raw[...], column(gk[...]), tab[:, : 4 * n])[: 3 * n]


def far_kernel(t3, t4, rawq, weight, gq, gk, tab, qt_ref, kv_ref, raw, raw_far):
    n = 2 * t3.shape[0]
    raw_far[n:, :] = jnp.zeros((128 - n, 128), jnp.bfloat16)
    made = dot(jnp.concatenate([t3[...], t4[...]], axis=0), weight[...]).astype(jnp.bfloat16)
    raw_far[:n, :] = made[:, 256:]
    kv_ref[...] = keys_values(raw_far[...], column(gk[...]), tab[:, 4 * n :])[:n]
    raw[: 3 * n, :] = rawq[...]
    raw[3 * n :, :] = made[:, :256]
    table = tab[:, : 4 * n]
    count = 4 * n
    for h in range(4):
        if h % 2 == 0:
            both = raw[:, h * 64 : h * 64 + 128].astype(jnp.float32).T
        x = both[(h % 2) * 64 : (h % 2) * 64 + 64]
        q = norm_turn(x, column(gq[h : h + 1, :]), table).astype(jnp.bfloat16)
        qt_ref[0:64, h * count : (h + 1) * count] = q
        qt_ref[64:128, h * count : (h + 1) * count] = jnp.zeros_like(q)


def join_kernel(*refs):
    *parts, out = refs
    at = 0
    for p in parts:
        out[at : at + p.shape[0], :] = p[...]
        at += p.shape[0]


def join(parts, size=None):
    size = size or parts[0].shape[0]
    rows = [min(size, p.shape[0]) for p in parts]
    specs = [pl.BlockSpec((r, 128), lambda i, b=p.shape[0] // r - 1: (b, 0)) for p, r in zip(parts, rows)]
    return pl.pallas_call(
        join_kernel,
        grid=(1,),
        out_shape=jax.ShapeDtypeStruct((sum(rows), 128), jnp.bfloat16),
        in_specs=specs,
        out_specs=pl.BlockSpec((sum(rows), 128), lambda i: (0, 0)),
        compiler_params=pltpu.CompilerParams(vmem_limit_bytes=4 * 2**20),
        cost_estimate=pl.CostEstimate(flops=1000, bytes_accessed=2**19, transcendentals=0),
    )(*parts)


def attend_kernel(*refs, n_kv, n_extra, first, last, scale, pieces):
    refs = list(refs)
    qt_ref = refs.pop(0)
    kv_refs = [refs.pop(0) for _ in range(n_kv)]
    extra = [refs.pop(0) for _ in range(n_extra)]
    if not first:
        acc_in, l_in, m_in = [refs.pop(0) for _ in range(3)]
    if last:
        att_refs = [refs.pop(0) for _ in range(4)]
        lse_ref = refs.pop(0)
        acc_ref, l_ref, m_ref = [refs.pop(0) for _ in range(3)]
    else:
        acc_ref, l_ref, m_ref = [refs.pop(0) for _ in range(3)]
    vt_ref, p_ref = refs
    c = scale * LOG2E
    nq = qt_ref.shape[1]

    def block(piece):
        parts = [kv_refs[j][r : r + size, :] for j, r, size in piece]
        return parts[0] if len(parts) == 1 else jnp.concatenate(parts, axis=0)

    for i, piece in enumerate(pieces):
        vt_ref[:, i * 384 : (i + 1) * 384] = block(piece).T[64:, :]

    for qi in range(nq // QT):
        cols = slice(qi * QT, (qi + 1) * QT)
        if first:
            top = None
            for piece in pieces:
                s = dot(block(piece)[:64], qt_ref[:, cols])
                s = jnp.max(s, axis=0, keepdims=True)
                top = s if top is None else jnp.maximum(top, s)
            m_ref[:, cols] = top * c + HEADROOM
            acc_ref[:, cols] = jnp.zeros((64, QT), jnp.float32)
            l_ref[:, cols] = jnp.zeros((8, QT), jnp.float32)
        else:
            m_ref[:, cols] = m_in[:, cols]
            acc_ref[:, cols] = acc_in[:, cols]
            l_ref[:, cols] = l_in[:, cols]

    def weigh(step, slot, cols):
        for h in range(2):
            s = dot(block(pieces[2 * step + h]), qt_ref[:, cols])
            p = jnp.exp2(s * c - m_ref[:, cols])
            l_ref[:, cols] += jnp.sum(p.reshape(48, 8, QT), axis=0)
            p_ref[slot, h * 384 : (h + 1) * 384, :] = p.astype(jnp.bfloat16)

    def gather_values(step, slot, cols):
        acc_ref[:, cols] += dot(vt_ref[:, step * 768 : (step + 1) * 768], p_ref[slot])

    steps = [
        (i, slice(qi * QT, (qi + 1) * QT)) for qi in range(nq // QT) for i in range(len(pieces) // 2)
    ]
    before = None
    for t, (i, cols) in enumerate(steps):
        weigh(i, t % 2, cols)
        if before is not None:
            gather_values(*before)
        before = (i, t % 2, cols)
    gather_values(*before)

    if last:
        total = jnp.sum(l_ref[...], axis=0, keepdims=True)
        good = jnp.logical_and(total > SUM_LOW, total < SUM_HIGH)
        n_bad = jnp.sum(jnp.where(good, 0.0, 1.0))

        @pl.when(n_bad > 0.0)
        def _():
            every = list(extra) + list(kv_refs)
            for qi in range(nq // 128):
                cols = slice(qi * 128, (qi + 1) * 128)
                m_ref[:, cols] = jnp.full((1, 128), -3e38, jnp.float32)
                acc_ref[:, cols] = jnp.zeros((64, 128), jnp.float32)
                l_ref[:, cols] = jnp.zeros((8, 128), jnp.float32)
            for kv in every:

                def top_of(i, _):
                    r = pl.multiple_of(i * 96, 96)
                    s = dot(kv[pl.ds(r, 96), :], qt_ref[...])
                    m_ref[...] = jnp.maximum(m_ref[...], jnp.max(s, axis=0, keepdims=True) * c)
                    return 0

                lax.fori_loop(0, kv.shape[0] // 96, top_of, 0)
            for kv in every:

                def again(i, _):
                    r = pl.multiple_of(i * 96, 96)
                    blk = kv[pl.ds(r, 96), :]
                    p = jnp.exp2(dot(blk, qt_ref[...]) * c - m_ref[...])
                    l_ref[...] += jnp.sum(p.reshape(12, 8, nq), axis=0)
                    acc_ref[...] += dot(blk.T[64:, :], p.astype(jnp.bfloat16))
                    return 0

                lax.fori_loop(0, kv.shape[0] // 96, again, 0)

        total = jnp.sum(l_ref[...], axis=0, keepdims=True)
        lse = (m_ref[...] + jnp.log2(total)) * (1.0 / LOG2E)
        out = acc_ref[...] / total
        count = nq // 4
        for h in range(0, 4, 2):
            two = jnp.concatenate(
                [out[:, h * count : (h + 1) * count], out[:, (h + 1) * count : (h + 2) * count]], axis=0
            )
            two = two.T.astype(jnp.bfloat16)
            for i, ref in enumerate(att_refs):
                ref[:, h * 64 : h * 64 + 128] = two[i * (count // 4) : (i + 1) * (count // 4)]
        for h in range(4):
            lse_ref[h : h + 1, :] = lse[:, h * count : (h + 1) * count]


def attend(qt, kvs, pieces, extra, state, last, scale):
    nq = qt.shape[1]
    keys = 384 * len(pieces)
    f32 = jnp.float32
    parts = (jax.ShapeDtypeStruct((64, nq), f32), jax.ShapeDtypeStruct((8, nq), f32), jax.ShapeDtypeStruct((1, nq), f32))
    scratch = [pltpu.VMEM((64, keys), jnp.bfloat16), pltpu.VMEM((2, KT, QT), jnp.bfloat16)]
    if last:
        outs = (jax.ShapeDtypeStruct((nq // 16, 256), jnp.bfloat16),) * 4 + (jax.ShapeDtypeStruct((4, nq // 4), f32),)
        scratch = [pltpu.VMEM(p.shape, f32) for p in parts] + scratch
    else:
        outs = parts
    args = [qt, *kvs, *extra, *(state or ())]
    return pl.pallas_call(
        functools.partial(
            attend_kernel, n_kv=len(kvs), n_extra=len(extra), first=state is None, last=last, scale=scale,
            pieces=pieces,
        ),
        out_shape=outs,
        in_specs=[VMEM] * len(args),
        out_specs=(VMEM,) * len(outs),
        scratch_shapes=scratch,
        compiler_params=pltpu.CompilerParams(vmem_limit_bytes=16 * 2**20),
        cost_estimate=pl.CostEstimate(
            flops=4 * nq * keys * 64, bytes_accessed=keys * 256 + nq * 512, transcendentals=nq * keys
        ),
    )(*args)


def mix_kernel(place, lse, a0, a1, a2, a3, w0, w1, w2, w3, x1, x2, x3, out_ref, lse_ref):
    half = w1.shape[0]
    here = pl.ds(pl.multiple_of(place[0] * half, half), half)
    there = pl.ds(pl.multiple_of((1 - place[0]) * half, half), half)
    total = dot(a0[...], w0[...])
    for a, w, x in ((a1, w1, x1), (a2, w2, x2), (a3, w3, x3)):
        total += dot(a[:, here], w[...]) + dot(a[:, there], x[...])
    out_ref[...] = total.astype(jnp.bfloat16)
    n = lse.shape[1] // 4
    cyc = [lse[:, i * n : (i + 1) * n] for i in (0, 2, 3, 1)]
    for t in range(4):

        @pl.when(place[1] == t)
        def _():
            lse_ref[...] = jnp.concatenate([cyc[(a - t) % 4] for a in range(4)], axis=1)


def body(tokens, query_weight, key_weight, value_weight, out_weight, query_gain, key_gain):
    scale = query_gain.shape[1] ** (-0.5)
    n = tokens.shape[0]
    sp, tp = lax.axis_index("sp"), lax.axis_index("tp")
    place = jnp.stack([sp & 1, tp])
    bf16 = jnp.bfloat16
    small = pltpu.CompilerParams(vmem_limit_bytes=12 * 2**20)

    def cost(tokens_done):
        return pl.CostEstimate(flops=2 * tokens_done * 2048 * 384, bytes_accessed=2**22, transcendentals=0)

    from_left = lax.ppermute(tokens, "tp", ring(4, 1))
    from_right = lax.ppermute(tokens, "tp", ring(4, 3))
    far_a = lax.ppermute(from_left[: n // 2], "tp", ring(4, 1))
    far_b = lax.ppermute(from_right[n // 2 :], "tp", ring(4, 3))
    table = angle_rows(sp, tp, n)
    half = out_weight.shape[0] // 2
    raw_own, weight, mine = pl.pallas_call(
        own_kernel,
        out_shape=(
            jax.ShapeDtypeStruct((n, 384), bf16),
            jax.ShapeDtypeStruct((2048, 384), bf16),
            jax.ShapeDtypeStruct((half, out_weight.shape[1]), bf16),
        ),
        in_specs=[pl.BlockSpec(memory_space=pltpu.SMEM)] + [VMEM] * 5,
        out_specs=(VMEM,) * 3,
        compiler_params=small,
        cost_estimate=cost(n),
    )(place, tokens, query_weight, key_weight.T, value_weight.T, out_weight)
    rawq, kv_near = pl.pallas_call(
        near_kernel,
        out_shape=(jax.ShapeDtypeStruct((3 * n, 256), bf16), jax.ShapeDtypeStruct((3 * n, 128), bf16)),
        in_specs=[VMEM] * 6,
        out_specs=(VMEM, VMEM),
        scratch_shapes=[pltpu.VMEM((4 * n, 128), bf16)],
        compiler_params=small,
        cost_estimate=cost(3 * n),
    )(raw_own, from_left, from_right, weight, key_gain, table)
    line = [kv_near]
    for k in (1, 3, 2):
        line.append(lax.ppermute(kv_near, "sp", grid_move(k, True)))
    qt, kv_far = pl.pallas_call(
        far_kernel,
        out_shape=(jax.ShapeDtypeStruct((128, 16 * n), bf16), jax.ShapeDtypeStruct((n, 128), bf16)),
        in_specs=[VMEM] * 7,
        out_specs=(VMEM, VMEM),
        scratch_shapes=[pltpu.VMEM((4 * n, 256), bf16), pltpu.VMEM((128, 128), bf16)],
        compiler_params=small,
        cost_estimate=cost(n),
    )(far_a, far_b, rawq, weight, query_gain, key_gain, table)

    load = join([*line, kv_far])
    twin = [lax.ppermute(load, "sp", core_swap())]
    got = [load]
    for k in (1, 3, 2):
        got.append(lax.ppermute(load, "sp", grid_move(k, False)))
    twin += [lax.ppermute(p, "sp", core_swap()) for p in got[1:]]
    line_far = join(got, n)
    rest = []
    for k in (1, 3, 2):
        rest.append(lax.ppermute(line_far, "sp", grid_move(k, True)))
    twin_rest = [lax.ppermute(p, "sp", core_swap()) for p in rest]

    mine, _ = lax.optimization_barrier((mine, kv_near))
    rows_in = []
    for k in (1, 3, 2):
        rows_in.append(lax.ppermute(mine, "tp", ring(4, k)))

    def thirds(j):
        return [((j, 384 * i, 384),) for i in range(3)]

    tails = tuple((j, 1152, 96) for j in range(4))
    state = attend(qt, [got[0], twin[0]], thirds(0) + thirds(1), [], None, False, scale)
    state = attend(qt, got, thirds(1) + thirds(2) + thirds(3) + [tails], [], state, False, scale)
    state = attend(qt, twin, thirds(1) + thirds(2) + thirds(3) + [tails], [], state, False, scale)
    *rows_in, _ = lax.optimization_barrier((*rows_in, state[2]))
    rows_other = [lax.ppermute(w, "sp", core_swap()) for w in rows_in]
    ends = [((j, 0, 384),) for j in range(6)]
    *att, lse = attend(qt, rest + twin_rest, ends, got + twin, state, True, scale)
    back = [lax.ppermute(att[i], "tp", ring(4, k)) for i, k in ((2, 1), (1, 3), (3, 2))]
    return pl.pallas_call(
        mix_kernel,
        out_shape=(jax.ShapeDtypeStruct((n, out_weight.shape[1]), bf16), jax.ShapeDtypeStruct((4, 4 * n), jnp.float32)),
        in_specs=[pl.BlockSpec(memory_space=pltpu.SMEM)] + [VMEM] * 12,
        out_specs=(VMEM, VMEM),
        compiler_params=small,
        cost_estimate=pl.CostEstimate(flops=2 * n * 1024 * 2048, bytes_accessed=2**22, transcendentals=0),
    )(place, lse, att[0], *back, out_weight, *rows_in, *rows_other)


def solution(mesh):
    return jax.shard_map(
        body,
        mesh=mesh,
        in_specs=(
            P(("sp", "tp"), None),
            P(None, "tp"),
            P(None, "tp"),
            P(None, "tp"),
            P("tp", None),
            P("tp", None),
            P("tp", None),
        ),
        out_specs=(P(("sp", "tp"), None), P("tp", "sp")),
        check_vma=False,
    )
```

```python
import functools

import jax
import jax.numpy as jnp
import numpy as np
from jax import lax
from jax.experimental import pallas as pl
from jax.experimental.pallas import tpu as pltpu
from jax.sharding import PartitionSpec as P


ROPE_BASE = 10000.0
LOG2E = 1.4426950408889634
HEADROOM = 40.0
SUM_LOW = 2.0**-80
SUM_HIGH = 2.0**100
VMEM = pl.BlockSpec(memory_space=pltpu.VMEM)
QT = 768
KT = 768


def ring(n, k):
    return [(i, (i + k) % n) for i in range(n)]


def grid_move(step, first):
    pairs = []
    for s in range(32):
        z, y, c = s // 8, (s // 2) % 4, s % 2
        if (c == 0) == first:
            z = (z + step) % 4
        else:
            y = (y + step) % 4
        pairs.append((s, z * 8 + y * 2 + c))
    return pairs


def core_swap():
    return [(s, s ^ 1) for s in range(32)]


def dot(a, b):
    return lax.dot_general(a, b, (((1,), (0,)), ((), ())), preferred_element_type=jnp.float32)


def angle_rows(sp, tp, n):
    lane = lax.broadcasted_iota(jnp.int32, (64, 4 * n), 1)
    row = lax.broadcasted_iota(jnp.int32, (64, 4 * n), 0)
    block = lax.div(lane, n)
    inside = lax.rem(lane, n)
    shift = jnp.where(block == 0, 0, jnp.where(block == 1, 3, jnp.where(block == 2, 1, 2)))
    place = sp * (4 * n) + ((tp + shift) & 3) * n + inside
    freq = jnp.asarray(np.tile(ROPE_BASE ** (-np.arange(16) / 16.0), 4)[:, None], jnp.float32)
    angle = jnp.where(row < 32, place >> 6, place & 63).astype(jnp.float32) * freq
    return jnp.where((row & 16) == 0, jnp.cos(angle), jnp.sin(angle))


def column(gain):
    eye = lax.broadcasted_iota(jnp.int32, (64, 64), 0) == lax.broadcasted_iota(jnp.int32, (64, 64), 1)
    wide = jnp.broadcast_to(gain.astype(jnp.float32), (64, 64))
    return jnp.sum(jnp.where(eye, wide, 0.0), axis=1, keepdims=True)


def norm_turn(x, gain, table):
    x = x * lax.rsqrt(jnp.mean(x * x, axis=0, keepdims=True) + 1e-06)
    x = x * gain
    rc, rs, cc, cs = table[0:16], table[16:32], table[32:48], table[48:64]
    a, b, c, d = x[0:16], x[16:32], x[32:48], x[48:64]
    return jnp.concatenate(
        [a * rc - b * rs, b * rc + a * rs, c * cc - d * cs, d * cc + c * cs], axis=0
    )


def keys_values(raw, gain, table):
    kv = raw.astype(jnp.float32).T
    keys = norm_turn(kv[0:64], gain, table)
    return jnp.concatenate([keys, kv[64:128]], axis=0).T.astype(jnp.bfloat16)


def own_kernel(place, t0, wq, wk, wv, wo, raw_ref, weight_ref, wo_ref):
    weight_ref[:, :256] = wq[...]
    weight_ref[:, 256:] = jnp.concatenate([wk[...], wv[...]], axis=0).astype(jnp.float32).T.astype(jnp.bfloat16)
    raw_ref[...] = dot(t0[...], weight_ref[...]).astype(jnp.bfloat16)
    half = wo_ref.shape[0]
    wo_ref[...] = wo[pl.ds(pl.multiple_of(place[0] * half, half), half), :]


def near_kernel(t1, t2, weight, raw_ref):
    n = t1.shape[0]
    for i, t in enumerate((t1, t2)):
        raw_ref[i * n : (i + 1) * n, :] = dot(t[...], weight[...]).astype(jnp.bfloat16)


def far_kernel(t3, t4, raw_own, raw_near, weight, gk, tab, kv_ref, raw_ref, raw):
    n = 2 * t3.shape[0]
    made = dot(jnp.concatenate([t3[...], t4[...]], axis=0), weight[...]).astype(jnp.bfloat16)
    for at, part in ((0, raw_own[...]), (n, raw_near[...]), (3 * n, made)):
        raw[at : at + part.shape[0], :] = part[:, 256:]
        raw_ref[at : at + part.shape[0], :] = part[:, :256]
    kv_ref[...] = keys_values(raw[...], column(gk[...]), tab[...])


def query_kernel(raw, gq, tab, qt_ref):
    count = raw.shape[0]
    table = tab[...]
    for h in range(4):
        if h % 2 == 0:
            both = raw[:, h * 64 : h * 64 + 128].astype(jnp.float32).T
        x = both[(h % 2) * 64 : (h % 2) * 64 + 64]
        q = norm_turn(x, column(gq[h : h + 1, :]), table).astype(jnp.bfloat16)
        qt_ref[0:64, h * count : (h + 1) * count] = q
        qt_ref[64:128, h * count : (h + 1) * count] = jnp.zeros_like(q)


def join_kernel(*refs):
    *parts, out = refs
    at = 0
    for p in parts:
        out[at : at + p.shape[0], :] = p[...]
        at += p.shape[0]


def join(parts):
    rows = sum(p.shape[0] for p in parts)
    return pl.pallas_call(
        join_kernel,
        out_shape=jax.ShapeDtypeStruct((rows, 128), jnp.bfloat16),
        in_specs=[VMEM] * len(parts),
        out_specs=VMEM,
        compiler_params=pltpu.CompilerParams(vmem_limit_bytes=4 * 2**20),
        cost_estimate=pl.CostEstimate(flops=1000, bytes_accessed=2**19, transcendentals=0),
    )(*parts)


def attend_kernel(*refs, n_kv, n_extra, first, last, scale, pieces):
    refs = list(refs)
    qt_ref = refs.pop(0)
    kv_refs = [refs.pop(0) for _ in range(n_kv)]
    extra = [refs.pop(0) for _ in range(n_extra)]
    if not first:
        acc_in, l_in, m_in = [refs.pop(0) for _ in range(3)]
    if last:
        att_refs = [refs.pop(0) for _ in range(4)]
        lse_ref = refs.pop(0)
        acc_ref, l_ref, m_ref = [refs.pop(0) for _ in range(3)]
    else:
        acc_ref, l_ref, m_ref = [refs.pop(0) for _ in range(3)]
    vt_ref, p_ref = refs
    c = scale * LOG2E
    nq = qt_ref.shape[1]

    def block(piece):
        parts = [kv_refs[j][r : r + size, :] for j, r, size in piece]
        return parts[0] if len(parts) == 1 else jnp.concatenate(parts, axis=0)

    for i, piece in enumerate(pieces):
        vt_ref[:, i * 384 : (i + 1) * 384] = block(piece).T[64:, :]

    for qi in range(nq // QT):
        cols = slice(qi * QT, (qi + 1) * QT)
        if first:
            top = None
            for piece in pieces:
                s = dot(block(piece)[:64], qt_ref[:, cols])
                s = jnp.max(s, axis=0, keepdims=True)
                top = s if top is None else jnp.maximum(top, s)
            m_ref[:, cols] = top * c + HEADROOM
            acc_ref[:, cols] = jnp.zeros((64, QT), jnp.float32)
            l_ref[:, cols] = jnp.zeros((8, QT), jnp.float32)
        else:
            m_ref[:, cols] = m_in[:, cols]
            acc_ref[:, cols] = acc_in[:, cols]
            l_ref[:, cols] = l_in[:, cols]

    def weigh(step, slot, cols):
        for h in range(2):
            s = dot(block(pieces[2 * step + h]), qt_ref[:, cols])
            p = jnp.exp2(s * c - m_ref[:, cols])
            l_ref[:, cols] += jnp.sum(p.reshape(48, 8, QT), axis=0)
            p_ref[slot, h * 384 : (h + 1) * 384, :] = p.astype(jnp.bfloat16)

    def gather_values(step, slot, cols):
        acc_ref[:, cols] += dot(vt_ref[:, step * 768 : (step + 1) * 768], p_ref[slot])

    steps = [
        (i, slice(qi * QT, (qi + 1) * QT)) for qi in range(nq // QT) for i in range(len(pieces) // 2)
    ]
    before = None
    for t, (i, cols) in enumerate(steps):
        weigh(i, t % 2, cols)
        if before is not None:
            gather_values(*before)
        before = (i, t % 2, cols)
    gather_values(*before)

    if last:
        total = jnp.sum(l_ref[...], axis=0, keepdims=True)
        good = jnp.logical_and(total > SUM_LOW, total < SUM_HIGH)
        n_bad = jnp.sum(jnp.where(good, 0.0, 1.0))

        @pl.when(n_bad > 0.0)
        def _():
            every = list(extra) + list(kv_refs)
            for qi in range(nq // 128):
                cols = slice(qi * 128, (qi + 1) * 128)
                m_ref[:, cols] = jnp.full((1, 128), -3e38, jnp.float32)
                acc_ref[:, cols] = jnp.zeros((64, 128), jnp.float32)
                l_ref[:, cols] = jnp.zeros((8, 128), jnp.float32)
            for kv in every:

                def top_of(i, _):
                    r = pl.multiple_of(i * 96, 96)
                    s = dot(kv[pl.ds(r, 96), :], qt_ref[...])
                    m_ref[...] = jnp.maximum(m_ref[...], jnp.max(s, axis=0, keepdims=True) * c)
                    return 0

                lax.fori_loop(0, kv.shape[0] // 96, top_of, 0)
            for kv in every:

                def again(i, _):
                    r = pl.multiple_of(i * 96, 96)
                    blk = kv[pl.ds(r, 96), :]
                    p = jnp.exp2(dot(blk, qt_ref[...]) * c - m_ref[...])
                    l_ref[...] += jnp.sum(p.reshape(12, 8, nq), axis=0)
                    acc_ref[...] += dot(blk.T[64:, :], p.astype(jnp.bfloat16))
                    return 0

                lax.fori_loop(0, kv.shape[0] // 96, again, 0)

        total = jnp.sum(l_ref[...], axis=0, keepdims=True)
        lse = (m_ref[...] + jnp.log2(total)) * (1.0 / LOG2E)
        out = acc_ref[...] / total
        count = nq // 4
        for h in range(0, 4, 2):
            two = jnp.concatenate(
                [out[:, h * count : (h + 1) * count], out[:, (h + 1) * count : (h + 2) * count]], axis=0
            )
            two = two.T.astype(jnp.bfloat16)
            for i, ref in enumerate(att_refs):
                ref[:, h * 64 : h * 64 + 128] = two[i * (count // 4) : (i + 1) * (count // 4)]
        for h in range(4):
            lse_ref[h : h + 1, :] = lse[:, h * count : (h + 1) * count]


def attend(qt, kvs, pieces, extra, state, last, scale):
    nq = qt.shape[1]
    keys = 384 * len(pieces)
    f32 = jnp.float32
    parts = (jax.ShapeDtypeStruct((64, nq), f32), jax.ShapeDtypeStruct((8, nq), f32), jax.ShapeDtypeStruct((1, nq), f32))
    scratch = [pltpu.VMEM((64, keys), jnp.bfloat16), pltpu.VMEM((2, KT, QT), jnp.bfloat16)]
    if last:
        outs = (jax.ShapeDtypeStruct((nq // 16, 256), jnp.bfloat16),) * 4 + (jax.ShapeDtypeStruct((4, nq // 4), f32),)
        scratch = [pltpu.VMEM(p.shape, f32) for p in parts] + scratch
    else:
        outs = parts
    args = [qt, *kvs, *extra, *(state or ())]
    return pl.pallas_call(
        functools.partial(
            attend_kernel, n_kv=len(kvs), n_extra=len(extra), first=state is None, last=last, scale=scale,
            pieces=pieces,
        ),
        out_shape=outs,
        in_specs=[VMEM] * len(args),
        out_specs=(VMEM,) * len(outs),
        scratch_shapes=scratch,
        compiler_params=pltpu.CompilerParams(vmem_limit_bytes=16 * 2**20),
        cost_estimate=pl.CostEstimate(
            flops=4 * nq * keys * 64, bytes_accessed=keys * 256 + nq * 512, transcendentals=nq * keys
        ),
    )(*args)


def early_kernel(place, lse, a0, w0, w1, w2, w3, x1, x2, x3, part_ref, rows_ref, lse_ref):
    half = w1.shape[0]
    part_ref[...] = dot(a0[...], w0[...])
    for i, (w, x) in enumerate(((w1, x1), (w2, x2), (w3, x3))):
        rows_ref[pl.ds(pl.multiple_of((2 * i + place[0]) * half, half), half), :] = w[...]
        rows_ref[pl.ds(pl.multiple_of((2 * i + 1 - place[0]) * half, half), half), :] = x[...]
    n = lse.shape[1] // 4
    cyc = [lse[:, i * n : (i + 1) * n] for i in (0, 2, 3, 1)]
    for t in range(4):

        @pl.when(place[1] == t)
        def _():
            lse_ref[...] = jnp.concatenate([cyc[(a - t) % 4] for a in range(4)], axis=1)


def mix_kernel(part, a1, a2, a3, rows, out_ref):
    both = jnp.concatenate([a1[...], a2[...], a3[...]], axis=1)
    out_ref[...] = (part[...] + dot(both, rows[...])).astype(jnp.bfloat16)


def body(tokens, query_weight, key_weight, value_weight, out_weight, query_gain, key_gain):
    scale = query_gain.shape[1] ** (-0.5)
    n = tokens.shape[0]
    sp, tp = lax.axis_index("sp"), lax.axis_index("tp")
    place = jnp.stack([sp & 1, tp])
    bf16 = jnp.bfloat16
    small = pltpu.CompilerParams(vmem_limit_bytes=12 * 2**20)

    def cost(tokens_done):
        return pl.CostEstimate(flops=2 * tokens_done * 2048 * 384, bytes_accessed=2**22, transcendentals=0)

    from_left = lax.ppermute(tokens, "tp", ring(4, 1))
    from_right = lax.ppermute(tokens, "tp", ring(4, 3))
    far_a = lax.ppermute(from_left[: n // 2], "tp", ring(4, 1))
    far_b = lax.ppermute(from_right[n // 2 :], "tp", ring(4, 3))
    table = angle_rows(sp, tp, n)
    half = out_weight.shape[0] // 2
    raw_own, weight, mine = pl.pallas_call(
        own_kernel,
        out_shape=(
            jax.ShapeDtypeStruct((n, 384), bf16),
            jax.ShapeDtypeStruct((2048, 384), bf16),
            jax.ShapeDtypeStruct((half, out_weight.shape[1]), bf16),
        ),
        in_specs=[pl.BlockSpec(memory_space=pltpu.SMEM)] + [VMEM] * 5,
        out_specs=(VMEM,) * 3,
        compiler_params=small,
        cost_estimate=cost(n),
    )(place, tokens, query_weight, key_weight.T, value_weight.T, out_weight)
    raw_near = pl.pallas_call(
        near_kernel,
        out_shape=jax.ShapeDtypeStruct((2 * n, 384), bf16),
        in_specs=[VMEM] * 3,
        out_specs=VMEM,
        compiler_params=small,
        cost_estimate=cost(2 * n),
    )(from_left, from_right, weight)
    kv, raw = pl.pallas_call(
        far_kernel,
        out_shape=(jax.ShapeDtypeStruct((4 * n, 128), bf16), jax.ShapeDtypeStruct((4 * n, 256), bf16)),
        in_specs=[VMEM] * 7,
        out_specs=(VMEM, VMEM),
        scratch_shapes=[pltpu.VMEM((4 * n, 128), bf16)],
        compiler_params=small,
        cost_estimate=cost(n),
    )(far_a, far_b, raw_own, raw_near, weight, key_gain, table)
    line = [kv]
    for k in (1, 3, 2):
        line.append(lax.ppermute(kv, "sp", grid_move(k, True)))
    qt = pl.pallas_call(
        query_kernel,
        out_shape=jax.ShapeDtypeStruct((128, 16 * n), bf16),
        in_specs=[VMEM] * 3,
        out_specs=VMEM,
        compiler_params=small,
        cost_estimate=cost(n),
    )(raw, query_gain, table)

    load = join(line)
    plane = []
    for k in (1, 3, 2):
        plane.append(lax.ppermute(load, "sp", grid_move(k, False)))
    load_twin = lax.ppermute(load, "sp", core_swap())
    plane_twin = []
    for k, p in zip((1, 3, 2), plane):
        plane_twin.append(lax.ppermute(p, "sp", core_swap()))

    mine, _ = lax.optimization_barrier((mine, kv))
    rows_in = []
    for k in (1, 3, 2):
        rows_in.append(lax.ppermute(mine, "tp", ring(4, k)))

    def quarters(j):
        return [((j, 384 * i, 384),) for i in range(4)]

    state = attend(qt, [load, load_twin], quarters(0) + quarters(1), [], None, False, scale)
    state = attend(qt, plane, quarters(0) + quarters(1) + quarters(2), [], state, False, scale)
    rows_in = lax.optimization_barrier((*rows_in, state[2]))[:3]
    rows_other = [lax.ppermute(w, "sp", core_swap()) for w in rows_in]
    *att, lse = attend(
        qt, plane_twin, quarters(0) + quarters(1) + quarters(2), [load, load_twin, *plane], state, True, scale
    )
    back = []
    for i, k in ((2, 1), (1, 3), (3, 2)):
        back.append(lax.ppermute(att[i], "tp", ring(4, k)))
    wide = out_weight.shape[1]
    part, rows, log_sums = pl.pallas_call(
        early_kernel,
        out_shape=(
            jax.ShapeDtypeStruct((n, wide), jnp.float32),
            jax.ShapeDtypeStruct((6 * half, wide), bf16),
            jax.ShapeDtypeStruct((4, 4 * n), jnp.float32),
        ),
        in_specs=[pl.BlockSpec(memory_space=pltpu.SMEM)] + [VMEM] * 9,
        out_specs=(VMEM,) * 3,
        compiler_params=small,
        cost_estimate=pl.CostEstimate(flops=2 * n * 256 * 2048, bytes_accessed=2**22, transcendentals=0),
    )(place, lse, att[0], out_weight, *rows_in, *rows_other)
    mixed = pl.pallas_call(
        mix_kernel,
        out_shape=jax.ShapeDtypeStruct((n, wide), bf16),
        in_specs=[VMEM] * 5,
        out_specs=VMEM,
        compiler_params=small,
        cost_estimate=pl.CostEstimate(flops=2 * n * 768 * 2048, bytes_accessed=2**22, transcendentals=0),
    )(part, *back, rows)
    return mixed, log_sums


def solution(mesh):
    return jax.shard_map(
        body,
        mesh=mesh,
        in_specs=(
            P(("sp", "tp"), None),
            P(None, "tp"),
            P(None, "tp"),
            P(None, "tp"),
            P("tp", None),
            P("tp", None),
            P("tp", None),
        ),
        out_specs=(P(("sp", "tp"), None), P("tp", "sp")),
        check_vma=False,
    )
```

```python
import functools

import jax
import jax.numpy as jnp
import numpy as np
from jax import lax
from jax.experimental import pallas as pl
from jax.experimental.pallas import tpu as pltpu
from jax.sharding import PartitionSpec as P


ROPE_BASE = 10000.0
LOG2E = 1.4426950408889634
HEADROOM = 40.0
SUM_LOW = 2.0**-80
SUM_HIGH = 2.0**100
VMEM = pl.BlockSpec(memory_space=pltpu.VMEM)
KT = 768
TILES_C = (768, 384)


def ring(n, k):
    return [(i, i ^ k) for i in range(n)]


def grid_move(step, first):
    pairs = []
    for s in range(32):
        z, y, c = s // 8, (s // 2) % 4, s % 2
        if (c == 0) == first:
            z ^= step
        else:
            y ^= step
        pairs.append((s, z * 8 + y * 2 + c))
    return pairs


def core_swap():
    return [(s, s ^ 1) for s in range(32)]


def dot(a, b):
    return lax.dot_general(a, b, (((1,), (0,)), ((), ())), preferred_element_type=jnp.float32)


def angle_rows(sp, tp, n):
    lane = lax.broadcasted_iota(jnp.int32, (64, 4 * n), 1)
    row = lax.broadcasted_iota(jnp.int32, (64, 4 * n), 0)
    block = lax.div(lane, n)
    inside = lax.rem(lane, n)
    shift = jnp.where(block == 0, 1, jnp.where(block == 1, 3, jnp.where(block == 2, 2, 0)))
    place = sp * (4 * n) + (tp ^ shift) * n + inside
    freq = jnp.asarray(np.tile(ROPE_BASE ** (-np.arange(16) / 16.0), 4)[:, None], jnp.float32)
    angle = jnp.where(row < 32, place >> 6, place & 63).astype(jnp.float32) * freq
    return jnp.where((row & 16) == 0, jnp.cos(angle), jnp.sin(angle))


def column(gain):
    eye = lax.broadcasted_iota(jnp.int32, (64, 64), 0) == lax.broadcasted_iota(jnp.int32, (64, 64), 1)
    wide = jnp.broadcast_to(gain.astype(jnp.float32), (64, 64))
    return jnp.sum(jnp.where(eye, wide, 0.0), axis=1, keepdims=True)


def norm_turn(x, gain, table):
    x = x * lax.rsqrt(jnp.mean(x * x, axis=0, keepdims=True) + 1e-06)
    x = x * gain
    rc, rs, cc, cs = table[0:16], table[16:32], table[32:48], table[48:64]
    a, b, c, d = x[0:16], x[16:32], x[32:48], x[48:64]
    return jnp.concatenate(
        [a * rc - b * rs, b * rc + a * rs, c * cc - d * cs, d * cc + c * cs], axis=0
    )


def keys_values(raw, gain, table):
    kv = raw.astype(jnp.float32).T
    keys = norm_turn(kv[0:64], gain, table)
    return jnp.concatenate([keys, kv[64:128]], axis=0).T.astype(jnp.bfloat16)


def own_kernel(place, t0, wq, wk, wv, wo, raw_ref, weight_ref, wo_ref):
    weight_ref[:, :256] = wq[...]
    weight_ref[:, 256:] = jnp.concatenate([wk[...], wv[...]], axis=0).astype(jnp.float32).T.astype(jnp.bfloat16)
    raw_ref[...] = dot(t0[...], weight_ref[...]).astype(jnp.bfloat16)
    half = wo_ref.shape[0]
    wo_ref[...] = wo[pl.ds(pl.multiple_of(place[0] * half, half), half), :]


def near_kernel(t1, t2, weight, raw_ref):
    n = t1.shape[0]
    for i, t in enumerate((t1, t2)):
        raw_ref[i * n : (i + 1) * n, :] = dot(t[...], weight[...]).astype(jnp.bfloat16)


def far_kernel(t3, t4, raw_own, raw_near, weight, gk, tab, kv_ref, raw_ref, raw):
    n = 2 * t3.shape[0]
    made = dot(jnp.concatenate([t3[...], t4[...]], axis=0), weight[...]).astype(jnp.bfloat16)
    for at, part in ((0, raw_near[...]), (2 * n, made), (3 * n, raw_own[...])):
        raw[at : at + part.shape[0], :] = part[:, 256:]
        raw_ref[at : at + part.shape[0], :] = part[:, :256]
    kv_ref[...] = keys_values(raw[...], column(gk[...]), tab[...])


def query_kernel(raw, gq, tab, qt_ref):
    count = raw.shape[0]
    n = count // 4
    table = tab[...]
    heads = []
    for h in range(4):
        if h % 2 == 0:
            both = raw[:, h * 64 : h * 64 + 128].astype(jnp.float32).T
        x = both[(h % 2) * 64 : (h % 2) * 64 + 64]
        heads.append(norm_turn(x, column(gq[h : h + 1, :]), table))
    for b in range(4):
        q = jnp.concatenate([x[:, b * n : (b + 1) * n] for x in heads], axis=1).astype(jnp.bfloat16)
        qt_ref[0:64, b * count : (b + 1) * count] = q
        qt_ref[64:128, b * count : (b + 1) * count] = jnp.zeros_like(q)


def join_kernel(*refs):
    *parts, out = refs
    at = 0
    for p in parts:
        out[at : at + p.shape[0], :] = p[...]
        at += p.shape[0]


def join(parts):
    rows = sum(p.shape[0] for p in parts)
    return pl.pallas_call(
        join_kernel,
        out_shape=jax.ShapeDtypeStruct((rows, 128), jnp.bfloat16),
        in_specs=[VMEM] * len(parts),
        out_specs=VMEM,
        compiler_params=pltpu.CompilerParams(vmem_limit_bytes=4 * 2**20),
        cost_estimate=pl.CostEstimate(flops=1000, bytes_accessed=2**19, transcendentals=0),
    )(*parts)


def attend_kernel(*refs, n_kv, n_extra, first, last, scale, pieces, span, tiles):
    refs = list(refs)
    qt_ref = refs.pop(0)
    kv_refs = [refs.pop(0) for _ in range(n_kv)]
    extra = [refs.pop(0) for _ in range(n_extra)]
    if not first:
        acc_in, l_in, m_in = [refs.pop(0) for _ in range(3)]
    if last:
        att_refs = [refs.pop(0) for _ in range((span[1] - span[0]) // 384)]
        lse_refs = [refs.pop(0) for _ in att_refs]
        acc_ref, l_ref, m_ref = [refs.pop(0) for _ in range(3)]
    else:
        acc_ref, l_ref, m_ref = [refs.pop(0) for _ in range(3)]
    vt_ref, p_ref = refs
    c = scale * LOG2E
    low, nq = span[0], span[1] - span[0]
    qt_ref = qt_ref.at[:, low : low + nq]

    def block(piece):
        parts = [kv_refs[j][r : r + size, :] for j, r, size in piece]
        return parts[0] if len(parts) == 1 else jnp.concatenate(parts, axis=0)

    for i, piece in enumerate(pieces):
        vt_ref[:, i * 384 : (i + 1) * 384] = block(piece).T[64:, :]

    ends = [sum(tiles[: i + 1]) for i in range(len(tiles))]
    columns = [slice(e - t, e) for e, t in zip(ends, tiles)]
    for cols in columns:
        QT = cols.stop - cols.start
        if first:
            top = None
            for piece in pieces:
                s = dot(block(piece)[:64], qt_ref[:, cols])
                s = jnp.max(s, axis=0, keepdims=True)
                top = s if top is None else jnp.maximum(top, s)
            m_ref[:, cols] = top * c + HEADROOM
            acc_ref[:, cols] = jnp.zeros((64, QT), jnp.float32)
            l_ref[:, cols] = jnp.zeros((8, QT), jnp.float32)
        else:
            m_ref[:, cols] = m_in[:, low + cols.start : low + cols.stop]
            acc_ref[:, cols] = acc_in[:, low + cols.start : low + cols.stop]
            l_ref[:, cols] = l_in[:, low + cols.start : low + cols.stop]

    def weigh(step, slot, cols):
        for h in range(2):
            s = dot(block(pieces[2 * step + h]), qt_ref[:, cols])
            p = jnp.exp2(s * c - m_ref[:, cols])
            l_ref[:, cols] += jnp.sum(p.reshape(48, 8, p.shape[1]), axis=0)
            p_ref[slot, h * 384 : (h + 1) * 384, : p.shape[1]] = p.astype(jnp.bfloat16)

    def gather_values(step, slot, cols):
        acc_ref[:, cols] += dot(vt_ref[:, step * 768 : (step + 1) * 768], p_ref[slot, :, : cols.stop - cols.start])

    steps = [(i, cols) for cols in columns for i in range(len(pieces) // 2)]
    before = None
    for t, (i, cols) in enumerate(steps):
        weigh(i, t % 2, cols)
        if before is not None:
            gather_values(*before)
        before = (i, t % 2, cols)
    gather_values(*before)

    if last:
        total = jnp.sum(l_ref[...], axis=0, keepdims=True)
        good = jnp.logical_and(total > SUM_LOW, total < SUM_HIGH)
        n_bad = jnp.sum(jnp.where(good, 0.0, 1.0))

        @pl.when(n_bad > 0.0)
        def _():
            every = list(extra) + list(kv_refs)
            for qi in range(nq // 128):
                cols = slice(qi * 128, (qi + 1) * 128)
                m_ref[:, cols] = jnp.full((1, 128), -3e38, jnp.float32)
                acc_ref[:, cols] = jnp.zeros((64, 128), jnp.float32)
                l_ref[:, cols] = jnp.zeros((8, 128), jnp.float32)
            for kv in every:

                def top_of(i, _):
                    r = pl.multiple_of(i * 96, 96)
                    s = dot(kv[pl.ds(r, 96), :], qt_ref[...])
                    m_ref[...] = jnp.maximum(m_ref[...], jnp.max(s, axis=0, keepdims=True) * c)
                    return 0

                lax.fori_loop(0, kv.shape[0] // 96, top_of, 0)
            for kv in every:

                def again(i, _):
                    r = pl.multiple_of(i * 96, 96)
                    blk = kv[pl.ds(r, 96), :]
                    p = jnp.exp2(dot(blk, qt_ref[...]) * c - m_ref[...])
                    l_ref[...] += jnp.sum(p.reshape(12, 8, nq), axis=0)
                    acc_ref[...] += dot(blk.T[64:, :], p.astype(jnp.bfloat16))
                    return 0

                lax.fori_loop(0, kv.shape[0] // 96, again, 0)

        total = jnp.sum(l_ref[...], axis=0, keepdims=True)
        lse = (m_ref[...] + jnp.log2(total)) * (1.0 / LOG2E)
        out = acc_ref[...] / total
        n = 96
        for b, (att_ref, lse_ref) in enumerate(zip(att_refs, lse_refs)):
            heads = [slice(b * 384 + h * n, b * 384 + (h + 1) * n) for h in range(4)]
            att_ref[...] = jnp.concatenate([out[:, h] for h in heads], axis=0).T.astype(jnp.bfloat16)
            lse_ref[...] = jnp.concatenate([lse[:, h] for h in heads], axis=0)


def attend(qt, kvs, pieces, extra, state, last, scale, span, tiles):
    nq = span[1] - span[0]
    keys = 384 * len(pieces)
    f32 = jnp.float32
    parts = (jax.ShapeDtypeStruct((64, nq), f32), jax.ShapeDtypeStruct((8, nq), f32), jax.ShapeDtypeStruct((1, nq), f32))
    scratch = [pltpu.VMEM((64, keys), jnp.bfloat16), pltpu.VMEM((2, KT, max(tiles)), jnp.bfloat16)]
    if last:
        blocks = nq // 384
        outs = (jax.ShapeDtypeStruct((96, 256), jnp.bfloat16),) * blocks + (jax.ShapeDtypeStruct((4, 96), f32),) * blocks
        scratch = [pltpu.VMEM(p.shape, f32) for p in parts] + scratch
    else:
        outs = parts
    args = [qt, *kvs, *extra, *(state or ())]
    return pl.pallas_call(
        functools.partial(
            attend_kernel, n_kv=len(kvs), n_extra=len(extra), first=state is None, last=last, scale=scale,
            pieces=pieces,
            span=span,
            tiles=tiles,
        ),
        out_shape=outs,
        in_specs=[VMEM] * len(args),
        out_specs=(VMEM,) * len(outs),
        scratch_shapes=scratch,
        compiler_params=pltpu.CompilerParams(vmem_limit_bytes=16 * 2**20),
        cost_estimate=pl.CostEstimate(
            flops=4 * nq * keys * 64, bytes_accessed=keys * 256 + nq * 512, transcendentals=nq * keys
        ),
    )(*args)


def early_kernel(place, s0, s1, s2, s3, a0, w0, w1, w2, w3, x1, x2, x3, part_ref, rows_ref, lse_ref):
    half = w1.shape[0]
    part_ref[...] = dot(a0[...], w0[...])
    for i, (w, x) in enumerate(((w1, x1), (w2, x2), (w3, x3))):
        rows_ref[pl.ds(pl.multiple_of((2 * i + place[0]) * half, half), half), :] = w[...]
        rows_ref[pl.ds(pl.multiple_of((2 * i + 1 - place[0]) * half, half), half), :] = x[...]
    sums = [s3[...], s0[...], s2[...], s1[...]]
    for t in range(4):

        @pl.when(place[1] == t)
        def _():
            lse_ref[...] = jnp.concatenate([sums[a ^ t] for a in range(4)], axis=1)


def mix_kernel(part, a1, a2, a3, rows, out_ref):
    both = jnp.concatenate([a1[...], a2[...], a3[...]], axis=1)
    out_ref[...] = (part[...] + dot(both, rows[...])).astype(jnp.bfloat16)


def body(tokens, query_weight, key_weight, value_weight, out_weight, query_gain, key_gain):
    scale = query_gain.shape[1] ** (-0.5)
    n = tokens.shape[0]
    sp, tp = lax.axis_index("sp"), lax.axis_index("tp")
    place = jnp.stack([sp & 1, tp])
    bf16 = jnp.bfloat16
    small = pltpu.CompilerParams(vmem_limit_bytes=12 * 2**20)

    def cost(tokens_done):
        return pl.CostEstimate(flops=2 * tokens_done * 2048 * 384, bytes_accessed=2**22, transcendentals=0)

    from_left = lax.ppermute(tokens, "tp", ring(4, 1))
    from_right = lax.ppermute(tokens, "tp", ring(4, 3))
    far_a = lax.ppermute(from_right[: n // 2], "tp", ring(4, 1))
    far_b = lax.ppermute(from_left[n // 2 :], "tp", ring(4, 3))
    table = angle_rows(sp, tp, n)
    half = out_weight.shape[0] // 2
    raw_own, weight, mine = pl.pallas_call(
        own_kernel,
        out_shape=(
            jax.ShapeDtypeStruct((n, 384), bf16),
            jax.ShapeDtypeStruct((2048, 384), bf16),
            jax.ShapeDtypeStruct((half, out_weight.shape[1]), bf16),
        ),
        in_specs=[pl.BlockSpec(memory_space=pltpu.SMEM)] + [VMEM] * 5,
        out_specs=(VMEM,) * 3,
        compiler_params=small,
        cost_estimate=cost(n),
    )(place, tokens, query_weight, key_weight.T, value_weight.T, out_weight)
    raw_near = pl.pallas_call(
        near_kernel,
        out_shape=jax.ShapeDtypeStruct((2 * n, 384), bf16),
        in_specs=[VMEM] * 3,
        out_specs=VMEM,
        compiler_params=small,
        cost_estimate=cost(2 * n),
    )(from_left, from_right, weight)
    kv, raw = pl.pallas_call(
        far_kernel,
        out_shape=(jax.ShapeDtypeStruct((4 * n, 128), bf16), jax.ShapeDtypeStruct((4 * n, 256), bf16)),
        in_specs=[VMEM] * 7,
        out_specs=(VMEM, VMEM),
        scratch_shapes=[pltpu.VMEM((4 * n, 128), bf16)],
        compiler_params=small,
        cost_estimate=cost(n),
    )(far_a, far_b, raw_own, raw_near, weight, key_gain, table)
    line = [kv]
    for k in (1, 3, 2):
        line.append(lax.ppermute(kv, "sp", grid_move(k, True)))
    qt = pl.pallas_call(
        query_kernel,
        out_shape=jax.ShapeDtypeStruct((128, 16 * n), bf16),
        in_specs=[VMEM] * 3,
        out_specs=VMEM,
        compiler_params=small,
        cost_estimate=cost(n),
    )(raw, query_gain, table)

    load = join(line)
    plane = []
    for k in (1, 3, 2):
        plane.append(lax.ppermute(load, "sp", grid_move(k, False)))
    load_twin = lax.ppermute(load, "sp", core_swap())
    plane_twin = []
    for k, p in zip((1, 3, 2), plane):
        plane_twin.append(lax.ppermute(p, "sp", core_swap()))

    mine, _ = lax.optimization_barrier((mine, kv))
    rows_in = []
    for k in (1, 3, 2):
        rows_in.append(lax.ppermute(mine, "tp", ring(4, k)))

    def quarters(j):
        return [((j, 384 * i, 384),) for i in range(4)]

    full, twice = (0, 16 * n), (768, 768)
    twelve = quarters(0) + quarters(1) + quarters(2)
    state = attend(qt, [load, load_twin], quarters(0) + quarters(1), [], None, False, scale, full, twice)
    state = attend(qt, plane, twelve, [], state, False, scale, full, twice)
    rows_in = lax.optimization_barrier((*rows_in, state[2]))[:3]
    rows_other = [lax.ppermute(w, "sp", core_swap()) for w in rows_in]
    others = [load, load_twin, *plane]
    *made, = attend(qt, plane_twin, twelve, others, state, True, scale, (0, 12 * n), TILES_C)
    att, sums = made[:3], made[3:]
    own, own_sums = attend(qt, plane_twin, twelve, others, state, True, scale, (12 * n, 16 * n), (384,))
    sums = [*sums, own_sums]
    back = []
    for i, k in ((0, 1), (1, 3), (2, 2)):
        back.append(lax.ppermute(att[i], "tp", ring(4, k)))
    wide = out_weight.shape[1]
    part, rows, log_sums = pl.pallas_call(
        early_kernel,
        out_shape=(
            jax.ShapeDtypeStruct((n, wide), jnp.float32),
            jax.ShapeDtypeStruct((6 * half, wide), bf16),
            jax.ShapeDtypeStruct((4, 4 * n), jnp.float32),
        ),
        in_specs=[pl.BlockSpec(memory_space=pltpu.SMEM)] + [VMEM] * 12,
        out_specs=(VMEM,) * 3,
        compiler_params=small,
        cost_estimate=pl.CostEstimate(flops=2 * n * 256 * 2048, bytes_accessed=2**22, transcendentals=0),
    )(place, *sums, own, out_weight, *rows_in, *rows_other)
    mixed = pl.pallas_call(
        mix_kernel,
        out_shape=jax.ShapeDtypeStruct((n, wide), bf16),
        in_specs=[VMEM] * 5,
        out_specs=VMEM,
        compiler_params=small,
        cost_estimate=pl.CostEstimate(flops=2 * n * 768 * 2048, bytes_accessed=2**22, transcendentals=0),
    )(part, *back, rows)
    return mixed, log_sums


def solution(mesh):
    return jax.shard_map(
        body,
        mesh=mesh,
        in_specs=(
            P(("sp", "tp"), None),
            P(None, "tp"),
            P(None, "tp"),
            P(None, "tp"),
            P("tp", None),
            P("tp", None),
            P("tp", None),
        ),
        out_specs=(P(("sp", "tp"), None), P("tp", "sp")),
        check_vma=False,
    )
```

```python
import functools

import jax
import jax.numpy as jnp
import numpy as np
from jax import lax
from jax.experimental import pallas as pl
from jax.experimental.pallas import tpu as pltpu
from jax.sharding import PartitionSpec as P


ROPE_BASE = 10000.0
LOG2E = 1.4426950408889634
HEADROOM = 40.0
SUM_LOW = 2.0**-80
SUM_HIGH = 2.0**100
VMEM = pl.BlockSpec(memory_space=pltpu.VMEM)
KT = 768
TILES_C = (768, 384)


def ring(n, k):
    return [(i, i ^ k) for i in range(n)]


def grid_move(step, first):
    pairs = []
    for s in range(32):
        z, y, c = s // 8, (s // 2) % 4, s % 2
        if (c == 0) == first:
            z ^= step
        else:
            y ^= step
        pairs.append((s, z * 8 + y * 2 + c))
    return pairs


def core_swap():
    return [(s, s ^ 1) for s in range(32)]


def dot(a, b):
    return lax.dot_general(a, b, (((1,), (0,)), ((), ())), preferred_element_type=jnp.float32)


def angle_rows(sp, tp, n):
    lane = lax.broadcasted_iota(jnp.int32, (64, 4 * n), 1)
    row = lax.broadcasted_iota(jnp.int32, (64, 4 * n), 0)
    block = lax.div(lane, n)
    inside = lax.rem(lane, n)
    shift = jnp.where(block == 0, 1, jnp.where(block == 1, 3, jnp.where(block == 2, 2, 0)))
    place = sp * (4 * n) + (tp ^ shift) * n + inside
    freq = jnp.asarray(np.tile(ROPE_BASE ** (-np.arange(16) / 16.0), 4)[:, None], jnp.float32)
    angle = jnp.where(row < 32, place >> 6, place & 63).astype(jnp.float32) * freq
    return jnp.where((row & 16) == 0, jnp.cos(angle), jnp.sin(angle))


def column(gain):
    eye = lax.broadcasted_iota(jnp.int32, (64, 64), 0) == lax.broadcasted_iota(jnp.int32, (64, 64), 1)
    wide = jnp.broadcast_to(gain.astype(jnp.float32), (64, 64))
    return jnp.sum(jnp.where(eye, wide, 0.0), axis=1, keepdims=True)


def norm_turn(x, gain, table):
    x = x * lax.rsqrt(jnp.mean(x * x, axis=0, keepdims=True) + 1e-06)
    x = x * gain
    rc, rs, cc, cs = table[0:16], table[16:32], table[32:48], table[48:64]
    a, b, c, d = x[0:16], x[16:32], x[32:48], x[48:64]
    return jnp.concatenate(
        [a * rc - b * rs, b * rc + a * rs, c * cc - d * cs, d * cc + c * cs], axis=0
    )


def keys_values(raw, gain, table):
    kv = raw.astype(jnp.float32).T
    keys = norm_turn(kv[0:64], gain, table)
    return jnp.concatenate([keys, kv[64:128]], axis=0).T.astype(jnp.bfloat16)


def own_kernel(place, t0, wq, wk, wv, wo, raw_ref, weight_ref, wo_ref):
    weight_ref[:, :256] = wq[...]
    weight_ref[:, 256:] = jnp.concatenate([wk[...], wv[...]], axis=0).astype(jnp.float32).T.astype(jnp.bfloat16)
    raw_ref[...] = dot(t0[...], weight_ref[...]).astype(jnp.bfloat16)
    half = wo_ref.shape[0]
    wo_ref[...] = wo[pl.ds(pl.multiple_of(place[0] * half, half), half), :]


def near_kernel(t1, t2, weight, raw_ref):
    n = t1.shape[0]
    for i, t in enumerate((t1, t2)):
        raw_ref[i * n : (i + 1) * n, :] = dot(t[...], weight[...]).astype(jnp.bfloat16)


def far_kernel(t3, t4, raw_own, raw_near, weight, gk, tab, kv_ref, raw_ref, raw):
    n = t3.shape[0] + t4.shape[0]
    made = dot(jnp.concatenate([t3[...], t4[...]], axis=0), weight[...]).astype(jnp.bfloat16)
    for at, part in ((0, raw_near[...]), (2 * n, made), (3 * n, raw_own[...])):
        raw[at : at + part.shape[0], :] = part[:, 256:]
        raw_ref[at : at + part.shape[0], :] = part[:, :256]
    kv_ref[...] = keys_values(raw[...], column(gk[...]), tab[...])


def query_kernel(raw, gq, tab, qt_ref):
    count = raw.shape[0]
    n = count // 4
    table = tab[...]
    heads = []
    for h in range(4):
        if h % 2 == 0:
            both = raw[:, h * 64 : h * 64 + 128].astype(jnp.float32).T
        x = both[(h % 2) * 64 : (h % 2) * 64 + 64]
        heads.append(norm_turn(x, column(gq[h : h + 1, :]), table))
    for b in range(4):
        q = jnp.concatenate([x[:, b * n : (b + 1) * n] for x in heads], axis=1).astype(jnp.bfloat16)
        qt_ref[0:64, b * count : (b + 1) * count] = q
        qt_ref[64:128, b * count : (b + 1) * count] = jnp.zeros_like(q)


def join_kernel(*refs):
    *parts, out = refs
    at = 0
    for p in parts:
        out[at : at + p.shape[0], :] = p[...]
        at += p.shape[0]


def join(parts):
    rows = sum(p.shape[0] for p in parts)
    return pl.pallas_call(
        join_kernel,
        out_shape=jax.ShapeDtypeStruct((rows, 128), jnp.bfloat16),
        in_specs=[VMEM] * len(parts),
        out_specs=VMEM,
        compiler_params=pltpu.CompilerParams(vmem_limit_bytes=4 * 2**20),
        cost_estimate=pl.CostEstimate(flops=1000, bytes_accessed=2**19, transcendentals=0),
    )(*parts)


def attend_kernel(*refs, n_kv, n_extra, first, last, scale, pieces, span, tiles):
    refs = list(refs)
    qt_ref = refs.pop(0)
    kv_refs = [refs.pop(0) for _ in range(n_kv)]
    extra = [refs.pop(0) for _ in range(n_extra)]
    if not first:
        acc_in, l_in, m_in = [refs.pop(0) for _ in range(3)]
    if last:
        att_refs = [refs.pop(0) for _ in range((span[1] - span[0]) // 384)]
        lse_refs = [refs.pop(0) for _ in att_refs]
        acc_ref, l_ref, m_ref = [refs.pop(0) for _ in range(3)]
    else:
        acc_ref, l_ref, m_ref = [refs.pop(0) for _ in range(3)]
    vt_ref, p_ref = refs
    c = scale * LOG2E
    low, nq = span[0], span[1] - span[0]
    qt_ref = qt_ref.at[:, low : low + nq]

    def block(piece):
        parts = [kv_refs[j][r : r + size, :] for j, r, size in piece]
        return parts[0] if len(parts) == 1 else jnp.concatenate(parts, axis=0)

    for i, piece in enumerate(pieces):
        vt_ref[:, i * 384 : (i + 1) * 384] = block(piece).T[64:, :]

    ends = [sum(tiles[: i + 1]) for i in range(len(tiles))]
    columns = [slice(e - t, e) for e, t in zip(ends, tiles)]
    for cols in columns:
        QT = cols.stop - cols.start
        if first:
            top = None
            for piece in pieces:
                s = dot(block(piece)[:64], qt_ref[:, cols])
                s = jnp.max(s, axis=0, keepdims=True)
                top = s if top is None else jnp.maximum(top, s)
            m_ref[:, cols] = top * c + HEADROOM
            acc_ref[:, cols] = jnp.zeros((64, QT), jnp.float32)
            l_ref[:, cols] = jnp.zeros((8, QT), jnp.float32)
        else:
            m_ref[:, cols] = m_in[:, low + cols.start : low + cols.stop]
            acc_ref[:, cols] = acc_in[:, low + cols.start : low + cols.stop]
            l_ref[:, cols] = l_in[:, low + cols.start : low + cols.stop]

    def weigh(step, slot, cols):
        for h in range(2):
            s = dot(block(pieces[2 * step + h]), qt_ref[:, cols])
            p = jnp.exp2(s * c - m_ref[:, cols])
            l_ref[:, cols] += jnp.sum(p.reshape(48, 8, p.shape[1]), axis=0)
            p_ref[slot, h * 384 : (h + 1) * 384, : p.shape[1]] = p.astype(jnp.bfloat16)

    def gather_values(step, slot, cols):
        acc_ref[:, cols] += dot(vt_ref[:, step * 768 : (step + 1) * 768], p_ref[slot, :, : cols.stop - cols.start])

    steps = [(i, cols) for cols in columns for i in range(len(pieces) // 2)]
    before = None
    for t, (i, cols) in enumerate(steps):
        weigh(i, t % 2, cols)
        if before is not None:
            gather_values(*before)
        before = (i, t % 2, cols)
    gather_values(*before)

    if last:
        total = jnp.sum(l_ref[...], axis=0, keepdims=True)
        good = jnp.logical_and(total > SUM_LOW, total < SUM_HIGH)
        n_bad = jnp.sum(jnp.where(good, 0.0, 1.0))

        @pl.when(n_bad > 0.0)
        def _():
            every = list(extra) + list(kv_refs)
            for qi in range(nq // 128):
                cols = slice(qi * 128, (qi + 1) * 128)
                m_ref[:, cols] = jnp.full((1, 128), -3e38, jnp.float32)
                acc_ref[:, cols] = jnp.zeros((64, 128), jnp.float32)
                l_ref[:, cols] = jnp.zeros((8, 128), jnp.float32)
            for kv in every:

                def top_of(i, _):
                    r = pl.multiple_of(i * 96, 96)
                    s = dot(kv[pl.ds(r, 96), :], qt_ref[...])
                    m_ref[...] = jnp.maximum(m_ref[...], jnp.max(s, axis=0, keepdims=True) * c)
                    return 0

                lax.fori_loop(0, kv.shape[0] // 96, top_of, 0)
            for kv in every:

                def again(i, _):
                    r = pl.multiple_of(i * 96, 96)
                    blk = kv[pl.ds(r, 96), :]
                    p = jnp.exp2(dot(blk, qt_ref[...]) * c - m_ref[...])
                    l_ref[...] += jnp.sum(p.reshape(12, 8, nq), axis=0)
                    acc_ref[...] += dot(blk.T[64:, :], p.astype(jnp.bfloat16))
                    return 0

                lax.fori_loop(0, kv.shape[0] // 96, again, 0)

        total = jnp.sum(l_ref[...], axis=0, keepdims=True)
        lse = (m_ref[...] + jnp.log2(total)) * (1.0 / LOG2E)
        out = acc_ref[...] / total
        n = 96
        for b, (att_ref, lse_ref) in enumerate(zip(att_refs, lse_refs)):
            heads = [slice(b * 384 + h * n, b * 384 + (h + 1) * n) for h in range(4)]
            att_ref[...] = jnp.concatenate([out[:, h] for h in heads], axis=0).T.astype(jnp.bfloat16)
            lse_ref[...] = jnp.concatenate([lse[:, h] for h in heads], axis=0)


def attend(qt, kvs, pieces, extra, state, last, scale, span, tiles):
    nq = span[1] - span[0]
    keys = 384 * len(pieces)
    f32 = jnp.float32
    parts = (jax.ShapeDtypeStruct((64, nq), f32), jax.ShapeDtypeStruct((8, nq), f32), jax.ShapeDtypeStruct((1, nq), f32))
    scratch = [pltpu.VMEM((64, keys), jnp.bfloat16), pltpu.VMEM((2, KT, max(tiles)), jnp.bfloat16)]
    if last:
        blocks = nq // 384
        outs = (jax.ShapeDtypeStruct((96, 256), jnp.bfloat16),) * blocks + (jax.ShapeDtypeStruct((4, 96), f32),) * blocks
        scratch = [pltpu.VMEM(p.shape, f32) for p in parts] + scratch
    else:
        outs = parts
    args = [qt, *kvs, *extra, *(state or ())]
    return pl.pallas_call(
        functools.partial(
            attend_kernel, n_kv=len(kvs), n_extra=len(extra), first=state is None, last=last, scale=scale,
            pieces=pieces,
            span=span,
            tiles=tiles,
        ),
        out_shape=outs,
        in_specs=[VMEM] * len(args),
        out_specs=(VMEM,) * len(outs),
        scratch_shapes=scratch,
        compiler_params=pltpu.CompilerParams(vmem_limit_bytes=16 * 2**20),
        cost_estimate=pl.CostEstimate(
            flops=4 * nq * keys * 64, bytes_accessed=keys * 256 + nq * 512, transcendentals=nq * keys
        ),
    )(*args)


def early_kernel(place, s0, s1, s2, s3, a0, w0, w1, w2, w3, x1, x2, x3, part_ref, rows_ref, lse_ref):
    half = w1.shape[0]
    part_ref[...] = dot(a0[...], w0[...])
    for i, (w, x) in enumerate(((w1, x1), (w2, x2), (w3, x3))):
        rows_ref[pl.ds(pl.multiple_of((2 * i + place[0]) * half, half), half), :] = w[...]
        rows_ref[pl.ds(pl.multiple_of((2 * i + 1 - place[0]) * half, half), half), :] = x[...]
    sums = [s3[...], s0[...], s2[...], s1[...]]
    for t in range(4):

        @pl.when(place[1] == t)
        def _():
            lse_ref[...] = jnp.concatenate([sums[a ^ t] for a in range(4)], axis=1)


def mix_kernel(part, a1, a2, a3, rows, out_ref):
    both = jnp.concatenate([a1[...], a2[...], a3[...]], axis=1)
    out_ref[...] = (part[...] + dot(both, rows[...])).astype(jnp.bfloat16)


def body(tokens, query_weight, key_weight, value_weight, out_weight, query_gain, key_gain):
    scale = query_gain.shape[1] ** (-0.5)
    n = tokens.shape[0]
    sp, tp = lax.axis_index("sp"), lax.axis_index("tp")
    place = jnp.stack([sp & 1, tp])
    bf16 = jnp.bfloat16
    small = pltpu.CompilerParams(vmem_limit_bytes=12 * 2**20)

    def cost(tokens_done):
        return pl.CostEstimate(flops=2 * tokens_done * 2048 * 384, bytes_accessed=2**22, transcendentals=0)

    from_left = lax.ppermute(tokens, "tp", ring(4, 1))
    from_right = lax.ppermute(tokens, "tp", ring(4, 3))
    far_a = lax.ppermute(from_right[: 2 * n // 3], "tp", ring(4, 1))
    far_b = lax.ppermute(from_left[2 * n // 3 :], "tp", ring(4, 3))
    table = angle_rows(sp, tp, n)
    half = out_weight.shape[0] // 2
    raw_own, weight, mine = pl.pallas_call(
        own_kernel,
        out_shape=(
            jax.ShapeDtypeStruct((n, 384), bf16),
            jax.ShapeDtypeStruct((2048, 384), bf16),
            jax.ShapeDtypeStruct((half, out_weight.shape[1]), bf16),
        ),
        in_specs=[pl.BlockSpec(memory_space=pltpu.SMEM)] + [VMEM] * 5,
        out_specs=(VMEM,) * 3,
        compiler_params=small,
        cost_estimate=cost(n),
    )(place, tokens, query_weight, key_weight.T, value_weight.T, out_weight)
    raw_near = pl.pallas_call(
        near_kernel,
        out_shape=jax.ShapeDtypeStruct((2 * n, 384), bf16),
        in_specs=[VMEM] * 3,
        out_specs=VMEM,
        compiler_params=small,
        cost_estimate=cost(2 * n),
    )(from_left, from_right, weight)
    kv, raw = pl.pallas_call(
        far_kernel,
        out_shape=(jax.ShapeDtypeStruct((4 * n, 128), bf16), jax.ShapeDtypeStruct((4 * n, 256), bf16)),
        in_specs=[VMEM] * 7,
        out_specs=(VMEM, VMEM),
        scratch_shapes=[pltpu.VMEM((4 * n, 128), bf16)],
        compiler_params=small,
        cost_estimate=cost(n),
    )(far_a, far_b, raw_own, raw_near, weight, key_gain, table)
    line = [kv]
    for k in (1, 3, 2):
        line.append(lax.ppermute(kv, "sp", grid_move(k, True)))
    qt = pl.pallas_call(
        query_kernel,
        out_shape=jax.ShapeDtypeStruct((128, 16 * n), bf16),
        in_specs=[VMEM] * 3,
        out_specs=VMEM,
        compiler_params=small,
        cost_estimate=cost(n),
    )(raw, query_gain, table)

    load = join(line)
    plane = []
    for k in (1, 3, 2):
        plane.append(lax.ppermute(load, "sp", grid_move(k, False)))
    load_twin = lax.ppermute(load, "sp", core_swap())
    plane_twin = []
    for k, p in zip((1, 3, 2), plane):
        plane_twin.append(lax.ppermute(p, "sp", core_swap()))

    mine, _ = lax.optimization_barrier((mine, kv))
    rows_in = []
    for k in (1, 3, 2):
        rows_in.append(lax.ppermute(mine, "tp", ring(4, k)))

    def quarters(j):
        return [((j, 384 * i, 384),) for i in range(4)]

    full, twice = (0, 16 * n), (768, 768)
    twelve = quarters(0) + quarters(1) + quarters(2)
    state = attend(qt, [load, load_twin], quarters(0) + quarters(1), [], None, False, scale, full, twice)
    state = attend(qt, plane, twelve, [], state, False, scale, full, twice)
    rows_in = lax.optimization_barrier((*rows_in, state[2]))[:3]
    rows_other = [lax.ppermute(w, "sp", core_swap()) for w in rows_in]
    others = [load, load_twin, *plane]
    *made, = attend(qt, plane_twin, twelve, others, state, True, scale, (0, 12 * n), TILES_C)
    att, sums = made[:3], made[3:]
    own, own_sums = attend(qt, plane_twin, twelve, others, state, True, scale, (12 * n, 16 * n), (384,))
    sums = [*sums, own_sums]
    back = []
    for i, k in ((0, 1), (1, 3), (2, 2)):
        back.append(lax.ppermute(att[i], "tp", ring(4, k)))
    wide = out_weight.shape[1]
    part, rows, log_sums = pl.pallas_call(
        early_kernel,
        out_shape=(
            jax.ShapeDtypeStruct((n, wide), jnp.float32),
            jax.ShapeDtypeStruct((6 * half, wide), bf16),
            jax.ShapeDtypeStruct((4, 4 * n), jnp.float32),
        ),
        in_specs=[pl.BlockSpec(memory_space=pltpu.SMEM)] + [VMEM] * 12,
        out_specs=(VMEM,) * 3,
        compiler_params=small,
        cost_estimate=pl.CostEstimate(flops=2 * n * 256 * 2048, bytes_accessed=2**22, transcendentals=0),
    )(place, *sums, own, out_weight, *rows_in, *rows_other)
    mixed = pl.pallas_call(
        mix_kernel,
        out_shape=jax.ShapeDtypeStruct((n, wide), bf16),
        in_specs=[VMEM] * 5,
        out_specs=VMEM,
        compiler_params=small,
        cost_estimate=pl.CostEstimate(flops=2 * n * 768 * 2048, bytes_accessed=2**22, transcendentals=0),
    )(part, *back, rows)
    return mixed, log_sums


def solution(mesh):
    return jax.shard_map(
        body,
        mesh=mesh,
        in_specs=(
            P(("sp", "tp"), None),
            P(None, "tp"),
            P(None, "tp"),
            P(None, "tp"),
            P("tp", None),
            P("tp", None),
            P("tp", None),
        ),
        out_specs=(P(("sp", "tp"), None), P("tp", "sp")),
        check_vma=False,
    )
```
